256 devices in a mesh: grp: 2 (over y), ep: 64 (over z, x), tp: 2 (over core).
Axes of the slice: x: 4, y: 2, z: 16, core: 2. Of those that a mesh axis runs over, the one named last changes fastest.
The devices are a block of a 4x16x16 slice.
Arguments:
- tokens: bfloat16 [32768, 2048], P(('grp', 'ep'), 'tp'), parts along dimension 0, may hold values from -6 to 6
- norm_gain: bfloat16 [2048], P('tp'), may hold values from 0.099609375 to 1.8984375
- w_gate: bfloat16 [64, 2048, 1024], P('ep', None, 'tp'), may hold values from -0.125 to 0.125
- w_up: bfloat16 [64, 2048, 1024], P('ep', None, 'tp'), may hold values from -0.125 to 0.125
- w_down: bfloat16 [64, 1024, 2048], P('ep', 'tp'), may hold values from -0.1875 to 0.1875
- expert_ids: int32 [32768, 2], P(('grp', 'ep')), parts along dimension 0, may hold values from 0 to 63, as said below
- combine: float32 [32768, 2], P(('grp', 'ep')), parts along dimension 0, may hold values from 0.1 to 1
- final_gain: bfloat16 [2048], P('tp'), may hold values from 0.099609375 to 1.8984375
Outputs:
- result: bfloat16 [32768, 2048], P(('grp', 'ep'), 'tp'), parts along dimension 0
The draws below stay inside these ranges and needn't reach their ends.
There are 2 independent parts, one for each index of `grp`. The reference program is written for one: setup_inputs(seed, part) draws one part's arguments, and reference() takes and returns one part's arrays. A program takes and returns all parts, laid end to end along the dimension named above; an argument that names none is the same for every part. Nothing has to cross between parts.
Inputs may be any that keep to these rules, and one draw needn't show every extreme that they name: `expert_ids`: the experts form 4 groups of consecutive ids of equal size; the 2 experts of a row are different and lie in one group. Among the rows of one index of ep no expert is named more than 20 times, and in each such block some expert is named exactly 20 times.
All inputs are finite; a program needn't handle non-finite values.
Results may differ from the reference program's by a relative error of at most 0.0077.
Values may be sent and summed in bfloat16 or wider, within the bound.
A program may use at most 64 MiB of HBM per device.

```python
import math
import jax
import jax.numpy as jnp
from jax import lax

D = 2048
FF = 1024
GROUPS = 4
TOP = 2
TOK_DEV = 256
EXPERTS = 64
CAP = 20
TOKENS = 16384
N_EP = 64
N_TP = 2


def draw_expert_ids(key, part):
    per_group = EXPERTS // GROUPS
    base = TOK_DEV // 8

    def one_block(block_key):
        key_busy, key_order, key_shift = jax.random.split(block_key, 3)
        busy = jax.random.randint(key_busy, (), 0, GROUPS)
        labels = jnp.arange(GROUPS, dtype=jnp.int32)
        counts = jnp.where(labels == busy, 5 * base, base).astype(jnp.int32)
        starts = jnp.cumsum(counts) - counts
        order = jax.random.permutation(key_order, TOK_DEV)
        ranks = jnp.arange(TOK_DEV, dtype=jnp.int32)
        group = jnp.sum((ranks[:, None] >= (starts + counts)[None, :]).astype(jnp.int32), axis=1)
        inner = ranks - starts[group]
        shifts = jax.random.randint(key_shift, (GROUPS,), 0, per_group)[group]
        first = (inner + shifts) % per_group
        second = (first + 1 + inner // per_group % max(per_group - 1, 1)) % per_group
        paired = jnp.stack([group * per_group + first, group * per_group + second], axis=1).astype(jnp.int32)
        return jnp.zeros((TOK_DEV, 2), jnp.int32).at[order].set(paired)
    blocks = jax.vmap(one_block)(jax.random.split(jax.random.fold_in(key, 11), TOKENS // TOK_DEV))
    return blocks.reshape(TOKENS, 2)


def block_scale(key, dims, cuts, low, high):
    loudness, own = 1.0, jax.random.fold_in(key, 6)
    for dim, blocks in cuts:
        steps = jnp.exp(jax.random.uniform(jax.random.fold_in(own, dim), (blocks,), jnp.float32, low / len(cuts), high / len(cuts)))
        loudness = loudness * jnp.repeat(steps, dims[dim] // blocks).reshape([-1 if axis == dim else 1 for axis in range(len(dims))])
    return loudness


def scatter_about(rng, dims, deviation, reach, cuts=(), held_as=jnp.bfloat16):
    array = deviation * jax.random.normal(rng, dims, jnp.float32)
    if cuts:
        array = array * block_scale(rng, dims, cuts, -0.22, 0.18)
    return jnp.clip(array, -reach, reach).astype(held_as)


def setup_inputs(seed: int = 0, part: int = 0) -> dict:
    key_of = jax.random.split(jax.random.key(seed), 9)
    own_keys = jax.random.split(jax.random.fold_in(key_of[8], part), 9)
    tokens = scatter_about(own_keys[0], (TOKENS, D), 1.0, 6.0, ((0, 64), (1, 2)))
    norm_gain = jnp.clip(1.0 + 0.18 * jax.random.normal(key_of[1], (D,), jnp.float32), 0.099609375, 1.8984375).astype(jnp.bfloat16)
    w_gate = scatter_about(key_of[2], (EXPERTS, D, FF), D ** -0.5, 0.125, ((0, 64), (2, 2)))
    w_up = scatter_about(key_of[3], (EXPERTS, D, FF), D ** -0.5, 0.125, ((0, 64), (2, 2)))
    w_down = scatter_about(key_of[4], (EXPERTS, FF, D), FF ** -0.5, 0.1875, ((0, 64), (1, 2)))
    expert_ids = draw_expert_ids(jax.random.fold_in(jax.random.fold_in(key_of[8], part), 71), part)
    combine = jnp.clip(jnp.exp(math.log(1.0) - 2.3025851 * jax.random.uniform(own_keys[6], (TOKENS, TOP), jnp.float32) ** block_scale(own_keys[6], (TOKENS, TOP), ((0, 64),), -0.2, 0.2)), 0.1, 1.0)
    final_gain = jnp.clip(1.0 + 0.18 * jax.random.normal(key_of[7], (D,), jnp.float32), 0.099609375, 1.8984375).astype(jnp.bfloat16)
    return dict(tokens=tokens, norm_gain=norm_gain, w_gate=w_gate, w_up=w_up, w_down=w_down, expert_ids=expert_ids, combine=combine, final_gain=final_gain)


def reference(tokens, norm_gain, w_gate, w_up, w_down, expert_ids, combine, final_gain):
    eps = 1e-06
    xf = tokens.astype(jnp.float32)
    normed = (xf * lax.rsqrt(lax.optimization_barrier(jnp.mean(xf * xf, axis=-1, keepdims=True)) + eps) * norm_gain.astype(jnp.float32)).astype(jnp.bfloat16)
    flat = expert_ids.reshape(-1)
    weights = combine.reshape(-1)
    limit = N_EP * CAP
    half_ff = FF // N_TP

    def step(acc, expert):
        hits = flat == expert
        pos = jnp.nonzero(hits, size=limit, fill_value=0)[0].astype(jnp.int32)
        live = jnp.arange(limit, dtype=jnp.int32) < jnp.sum(hits.astype(jnp.int32))
        owner = pos // TOP
        rows = normed[owner].astype(jnp.float32)
        gate_w = lax.dynamic_index_in_dim(w_gate, expert, 0, keepdims=False).astype(jnp.float32)
        up_w = lax.dynamic_index_in_dim(w_up, expert, 0, keepdims=False).astype(jnp.float32)
        down_w = lax.dynamic_index_in_dim(w_down, expert, 0, keepdims=False).astype(jnp.float32)
        gate = jnp.dot(rows, gate_w, preferred_element_type=jnp.float32)
        upper = jnp.dot(rows, up_w, preferred_element_type=jnp.float32)
        hidden = (jax.nn.silu(gate) * upper).astype(jnp.bfloat16)
        parts = jnp.einsum('rjf,jfd->jrd', hidden.astype(jnp.float32).reshape(limit, N_TP, half_ff), down_w.reshape(N_TP, half_ff, D)).astype(jnp.bfloat16)
        parts = lax.optimization_barrier(parts)
        summed = lax.optimization_barrier(jnp.sum(parts.astype(jnp.float32), axis=0)).astype(jnp.bfloat16)
        summed = lax.optimization_barrier(summed)
        scale = jnp.where(live, weights[pos], jnp.float32(0.0))
        acc = acc.at[owner].add(scale[:, None] * summed.astype(jnp.float32))
        return (acc, None)
    mixed, _ = lax.scan(step, jnp.zeros((TOKENS, D), jnp.float32), jnp.arange(EXPERTS, dtype=jnp.int32))
    norm = lax.rsqrt(lax.optimization_barrier(jnp.mean(mixed * mixed, axis=-1, keepdims=True)) + eps)
    return (mixed * norm * final_gain.astype(jnp.float32)).astype(jnp.bfloat16)
```

```python
import functools

import jax
import jax.numpy as jnp
from jax import lax
from jax.experimental import pallas as pl
from jax.experimental.pallas import tpu as pltpu
from jax.sharding import PartitionSpec as P

GROUPS = 4
SHORT = 4
ROWS = 16
EPS = 1e-06
MESH = pl.DeviceIdType.MESH
F32 = jnp.float32
BF16 = jnp.bfloat16


def dot(a, b):
    return jnp.dot(a, b, preferred_element_type=F32)


def kernel(
    X, nz, slots,
    tok_ref, note_ref, first_gain, last_gain, gate_hbm, up_hbm, down_hbm,
    out_ref,
    blocks, notes, packs, rows, others, given, taken, done, back, mix, sums, total,
    before, sq_out, sq_in, gate_w, up_w, down_w,
    load_sem, ring_s, ring_r, note_s, note_r, pack_s, pack_r, half_s, half_r,
    part_s, part_r, back_s, back_r, sum_s, sum_r, sq_s, sq_r,
):
    T, half = tok_ref.shape
    C = T // 2
    H = nz // 2
    width = 2 * half
    ep = lax.axis_index("ep")
    tp = lax.axis_index("tp")
    z, x = ep // X, ep % X
    mate = 1 - tp
    ahead = lax.rem(z + 1 - 2 * tp + nz, nz) * X + x
    behind = lax.rem(z - 1 + 2 * tp + nz, nz) * X + x

    def peer(d):
        return lax.rem(x + d, X)

    barrier = pltpu.get_barrier_semaphore()
    for other in [ahead, behind] + [z * X + peer(d) for d in range(1, X)]:
        pl.semaphore_signal(barrier, inc=1, device_id={"ep": other}, device_id_type=MESH)
    pl.semaphore_signal(barrier, inc=1, device_id={"tp": mate}, device_id_type=MESH)

    loads = [
        pltpu.make_async_copy(gate_hbm.at[0], gate_w, load_sem.at[0]),
        pltpu.make_async_copy(up_hbm.at[0], up_w, load_sem.at[1]),
        pltpu.make_async_copy(down_hbm.at[0], down_w, load_sem.at[2]),
    ]
    for load in loads:
        load.start()

    def to_mate(src, dst, s, r):
        return pltpu.make_async_remote_copy(
            src_ref=src, dst_ref=dst, send_sem=s, recv_sem=r,
            device_id={"tp": mate}, device_id_type=MESH,
        )

    def to_ep(src, dst, s, r, other):
        return pltpu.make_async_remote_copy(
            src_ref=src, dst_ref=dst, send_sem=s, recv_sem=r,
            device_id={"ep": other}, device_id_type=MESH,
        )

    def sq_copy(n):
        return to_mate(sq_out.at[n], sq_in.at[n], sq_s.at[n], sq_r.at[n])

    def landing(way, k):
        return jnp.minimum(2 * k - 1 + tp, nz - 1) if way == 0 else 2 * k - tp

    def source(way, k):
        return jnp.where(k == 1, 0, landing(way, k - 1))

    def neighbour(way):
        return ahead if way == 0 else behind

    def ring(way, k, c):
        return to_ep(
            blocks.at[source(way, k), c], blocks.at[landing(way, k), c],
            ring_s.at[way, k - 1, c], ring_r.at[way, k - 1, c], neighbour(way),
        )

    def note(way, k):
        return to_ep(
            notes.at[source(way, k)], notes.at[landing(way, k)],
            note_s.at[way, k - 1], note_r.at[way, k - 1], neighbour(way),
        )

    def pack(b, d):
        return to_ep(
            packs.at[b, peer(d)], rows.at[b, x],
            pack_s.at[b, peer(d)], pack_r.at[b, x], z * X + peer(d),
        )

    def pack_in(b, d):
        return to_ep(
            packs.at[b, peer(d)], rows.at[b, peer(d)],
            pack_s.at[b, peer(d)], pack_r.at[b, peer(d)], z * X + peer(d),
        )

    def half_copy(b):
        return to_mate(rows.at[b], others.at[b], half_s.at[b], half_r.at[b])

    def part_copy(b):
        return to_mate(given.at[b], taken.at[b], part_s.at[b], part_r.at[b])

    def home(b, d):
        return to_ep(
            done.at[b, peer(d)], back.at[b, x],
            back_s.at[b, peer(d)], back_r.at[b, x], z * X + peer(d),
        )

    def home_in(b, d):
        return to_ep(
            done.at[b, peer(d)], back.at[b, peer(d)],
            back_s.at[b, peer(d)], back_r.at[b, peer(d)], z * X + peer(d),
        )

    def sum_copy(way, k, c):
        return to_ep(
            blocks.at[landing(way, k), c], sums.at[way, k - 1, c],
            sum_s.at[way, k - 1, c], sum_r.at[way, k - 1, c], neighbour(1 - way),
        )

    narrow = tok_ref[...].astype(F32)
    own = jnp.broadcast_to(jnp.sum(narrow * narrow, axis=1, keepdims=True), (T, 128))
    sq_out[0] = own
    notes[0] = note_ref[...]
    below = lax.broadcasted_iota(jnp.int32, (T, T), 0) < lax.broadcasted_iota(jnp.int32, (T, T), 1)
    before[...] = below.astype(F32).astype(BF16)
    pl.semaphore_wait(barrier, X + 2)
    sq_copy(0).start()
    sq_copy(0).wait_recv()
    scale = lax.rsqrt((sq_out[0] + sq_in[0])[:, :1] / width + EPS)
    normed = tok_ref[...].astype(F32) * scale * first_gain[...].astype(F32)
    blocks[0] = normed.astype(BF16).reshape(2, C, half)

    def step(i, carry):
        k, c = i // 2, i % 2
        for way in range(2):
            last = H - way

            @pl.when((k >= 1) & (k <= last))
            def _():
                @pl.when(c == 0)
                def _():
                    note(way, k).wait_recv()

                ring(way, k, c).wait_recv()

            @pl.when(k < last)
            def _():
                @pl.when(c == 0)
                def _():
                    note(way, k + 1).start()

                ring(way, k + 1, c).start()

        @pl.when((i >= 2) & (i < nz + 2))
        def _():
            b = i - 2
            tag = notes[b]
            ids = (lax.broadcasted_iota(jnp.int32, (8, T), 0) + z * X).astype(F32)
            first, second = tag[0:1] == ids, tag[1:2] == ids
            hit = first | second
            rank = dot(hit.astype(F32).astype(BF16), before[...])
            key = jnp.where(hit, rank, -1.0)
            weight = jnp.where(first, tag[2:3], 0.0) + jnp.where(second, tag[3:4], 0.0)
            place = lax.broadcasted_iota(jnp.int32, (slots, T), 0).astype(F32)
            chosen, scaled = [], []
            for e in range(X):
                mark = key[e : e + 1] == place
                chosen.append(mark.astype(F32).astype(BF16))
                scaled.append(jnp.where(mark, weight[e : e + 1], 0.0))
            pick = jnp.concatenate(chosen, axis=0)
            spread = jnp.concatenate(scaled, axis=0).T
            high = spread.astype(BF16)
            low = (spread - high.astype(F32)).astype(BF16)
            mix[b] = jnp.concatenate([high, low], axis=1).reshape(2, C, 2 * X * slots)
            packs[b] = dot(pick, blocks[b].reshape(T, half)).astype(BF16).reshape(X, slots, half)
            rows[b, x] = packs[b, x]
            for d in range(1, X):
                pack(b, d).start()

        @pl.when((i >= 3) & (i < nz + 3))
        def _():
            b = i - 3
            for d in range(1, X):
                pack_in(b, d).wait_recv()
            half_copy(b).start()

        @pl.when(i == 4)
        def _():
            for load in loads:
                load.wait()

        @pl.when((i >= 4) & (i < nz + 4))
        def _():
            b = i - 4
            half_copy(b).wait_recv()
            mine = rows[b].reshape(X * slots, half)
            other = others[b].reshape(X * slots, half)
            near = pl.ds(pl.multiple_of(tp * half, half), half)
            far = pl.ds(pl.multiple_of(mate * half, half), half)
            gate = dot(mine, gate_w[near, :]) + dot(other, gate_w[far, :])
            upper = dot(mine, up_w[near, :]) + dot(other, up_w[far, :])
            hidden = (gate / (1.0 + jnp.exp(-gate)) * upper).astype(BF16)
            given[b] = dot(hidden, down_w[:, far]).astype(BF16).reshape(X, slots, half)
            part_copy(b).start()
            done[b] = dot(hidden, down_w[:, near]).astype(BF16).reshape(X, slots, half)

        @pl.when(i >= 5)
        def _():
            b = i - 5
            part_copy(b).wait_recv()
            done[b] = (done[b].astype(F32) + taken[b].astype(F32)).astype(BF16)
            for d in range(1, X):
                home(b, d).start()
            back[b, x] = done[b, x]

        return carry

    lax.fori_loop(0, nz + 5, step, 0)

    def drain(n, carry):
        for way in range(2):

            @pl.when(n < H - way)
            def _():
                note(way, n + 1).wait_send()
                for c in range(2):
                    ring(way, n + 1, c).wait_send()

        for d in range(1, X):
            pack(n, d).wait_send()
        half_copy(n).wait_send()
        part_copy(n).wait_send()
        return carry

    lax.fori_loop(0, nz, drain, 0)

    def arrive(b):
        for d in range(1, X):
            home_in(b, d).wait_recv()

    def share(b, c):
        made = back[b].reshape(X * slots, half)
        return dot(mix[b, c], jnp.concatenate([made, made], axis=0))

    def unwind(i, carry):
        j, c = i // 2, i % 2
        for way in range(2):
            last = H - way
            k = last - j
            b = landing(way, k)

            @pl.when((k >= 1) & (c == 0))
            def _():
                arrive(b)

            @pl.when(k == last)
            def _():
                blocks[b, c] = share(b, c).astype(BF16)
                sum_copy(way, k, c).start()

            @pl.when((k >= 1) & (k < last))
            def _():
                part = share(b, c)
                sum_copy(way, k + 1, c).wait_recv()
                blocks[b, c] = (part + sums[way, k, c].astype(F32)).astype(BF16)
                sum_copy(way, k, c).start()

        return carry

    lax.fori_loop(0, 2 * H, unwind, 0)

    arrive(0)
    for c in range(2):
        part = share(0, c)
        for way in range(2):
            sum_copy(way, 1, c).wait_recv()
        mixed = part + sums[0, 0, c].astype(F32) + sums[1, 0, c].astype(F32)
        total[c] = mixed
        sq_out[1, pl.ds(c * C, C), :] = jnp.broadcast_to(
            jnp.sum(mixed * mixed, axis=1, keepdims=True), (C, 128)
        )
    sq_copy(1).start()
    sq_copy(1).wait_recv()
    norm = lax.rsqrt((sq_out[1] + sq_in[1])[:, :1] / width + EPS)
    out_ref[...] = (total[...].reshape(T, half) * norm * last_gain[...].astype(F32)).astype(BF16)

    for n in range(2):
        sq_copy(n).wait_send()

    def finish(n, carry):
        for d in range(1, X):
            home(n, d).wait_send()
        for way in range(2):

            @pl.when(n < H - way)
            def _():
                for c in range(2):
                    sum_copy(way, n + 1, c).wait_send()

        return carry

    lax.fori_loop(0, nz, finish, 0)


def body(tokens, norm_gain, w_gate, w_up, w_down, expert_ids, combine, final_gain, X=SHORT):
    T, half = tokens.shape
    n_ep = lax.axis_size("ep")
    nz = n_ep // X
    H = nz // 2
    per_group = n_ep * w_gate.shape[0] // GROUPS
    capacity = T // 8 * 5 * 2 // per_group
    slots = -(-capacity // ROWS) * ROWS
    hidden = w_gate.shape[2]
    C = T // 2
    note = jnp.concatenate(
        [expert_ids.T.astype(F32), combine.T, jnp.zeros((4, T), F32)], axis=0
    )
    piece = (nz, X, slots, half)
    vmem = pl.BlockSpec(memory_space=pltpu.VMEM)
    hbm = pl.BlockSpec(memory_space=pl.ANY)
    dma = pltpu.SemaphoreType.DMA
    return pl.pallas_call(
        functools.partial(kernel, X, nz, slots),
        out_shape=jax.ShapeDtypeStruct((T, half), BF16),
        in_specs=[vmem] * 4 + [hbm] * 3,
        out_specs=vmem,
        scratch_shapes=[
            pltpu.VMEM((nz, 2, C, half), BF16),
            pltpu.VMEM((nz, 8, T), F32),
            pltpu.VMEM(piece, BF16),
            pltpu.VMEM(piece, BF16),
            pltpu.VMEM(piece, BF16),
            pltpu.VMEM(piece, BF16),
            pltpu.VMEM(piece, BF16),
            pltpu.VMEM(piece, BF16),
            pltpu.VMEM(piece, BF16),
            pltpu.VMEM((nz, 2, C, 2 * X * slots), BF16),
            pltpu.VMEM((2, H, 2, C, half), BF16),
            pltpu.VMEM((2, C, half), F32),
            pltpu.VMEM((T, T), BF16),
            pltpu.VMEM((2, T, 128), F32),
            pltpu.VMEM((2, T, 128), F32),
            pltpu.VMEM((2 * half, hidden), BF16),
            pltpu.VMEM((2 * half, hidden), BF16),
            pltpu.VMEM((hidden, 2 * half), BF16),
            dma((3,)),
            dma((2, H, 2)),
            dma((2, H, 2)),
            dma((2, H)),
            dma((2, H)),
            dma((nz, X)),
            dma((nz, X)),
            dma((nz,)),
            dma((nz,)),
            dma((nz,)),
            dma((nz,)),
            dma((nz, X)),
            dma((nz, X)),
            dma((2, H, 2)),
            dma((2, H, 2)),
            dma((2,)),
            dma((2,)),
        ],
        compiler_params=pltpu.CompilerParams(
            collective_id=0, has_side_effects=True, vmem_limit_bytes=62 * 1024 * 1024
        ),
    )(tokens, note, norm_gain.reshape(1, half), final_gain.reshape(1, half), w_gate, w_up, w_down)


def solution(mesh):
    placed = (
        P(("grp", "ep"), "tp"),
        P("tp"),
        P("ep", None, "tp"),
        P("ep", None, "tp"),
        P("ep", "tp", None),
        P(("grp", "ep"), None),
        P(("grp", "ep"), None),
        P("tp"),
    )
    return jax.shard_map(
        body, mesh=mesh, in_specs=placed, out_specs=P(("grp", "ep"), "tp"), check_vma=False
    )
```
